256 devices in a mesh: kv: 32 (over z, y), tp: 8 (over x, core).
Axes of the slice: x: 4, y: 4, z: 8, core: 2. Of those that a mesh axis runs over, the one named last changes fastest.
Arguments:
- tokens: bfloat16 [32, 6, 2048], replicated, may hold values from -6 to 6
- in_gain: bfloat16 [2048], replicated, may hold values from 0.099609375 to 1.8984375
- w_down_q: bfloat16 [2048, 512], P('kv'), may hold values from -0.125 to 0.125
- w_down_kv: bfloat16 [2048, 256], P('kv'), may hold values from -0.125 to 0.125
- w_rope_key: bfloat16 [2048, 32], replicated, may hold values from -0.125 to 0.125
- q_gain: bfloat16 [512], replicated, may hold values from 0.099609375 to 1.8984375
- kv_gain: bfloat16 [256], replicated, may hold values from 0.099609375 to 1.8984375
- w_up_q: bfloat16 [512, 1536], P(None, 'tp'), may hold values from -0.25 to 0.25
- w_absorb: bfloat16 [16, 64, 256], P('tp'), may hold values from -0.75 to 0.75
- w_value: bfloat16 [256, 1024], P(None, 'tp'), may hold values from -0.375 to 0.375
- w_out: bfloat16 [1024, 2048], P('tp'), may hold values from -0.1875 to 0.1875
- out_gain: bfloat16 [2048], replicated, may hold values from 0.099609375 to 1.8984375
- cache: bfloat16 [32, 65536, 288], P(None, 'kv'), may hold values from -1300 to 1300
- cached: int32 [32], replicated, may hold values from 1 to 65524, as said below
- accepted: int32 [32], replicated, may hold values from 0 to 6
- parents: int32 [32, 6], replicated, may hold values from -1 to 4, as said below
Outputs:
- attended: bfloat16 [32, 6, 2048], P('tp')
- new_cache: bfloat16 [32, 65536, 288], P(None, 'kv')
The draws below stay inside these ranges and needn't reach their ends.
Inputs may be any that keep to these rules, and one draw needn't show every extreme that they name: Some sequence has at least 64512 cached positions and some has at most 12. parents[s, j] is -1 or less than j.
All inputs are finite; a program needn't handle non-finite values.
Results may differ from the reference program's by a relative error of at most 0.023.
The reference program's roundings to bfloat16 on the way (of `normed`, `query_in`, `latent`, `rope_key`, `query_lat`, `lat_out` and `head_out`) count: a program that leaves them out, or rounds other values in their place, can miss the bound.
Values may be sent and summed in bfloat16 or wider, within the bound.
A program may use at most 320 MiB of HBM per device.

```python
import jax
import jax.numpy as jnp
from jax import lax

D = 2048
Q_RANK = 512
KV_RANK = 256
HEADS = 16
NOPE = 64
ROPE = 32
VDIM = 64
PROP = 6
SEQS = 32
CTX_DEV = 2048
CTX = 65536
N_KV = 32
N_TP = 8


def shared_lengths(key):
    top_len = CTX - 2 * PROP
    powers = jax.random.randint(jax.random.fold_in(key, 21), (SEQS,), 1, top_len.bit_length() + 1)
    ceiling = jnp.minimum(jnp.left_shift(jnp.ones((SEQS,), jnp.int32), powers), top_len)
    lengths = jax.random.randint(jax.random.fold_in(key, 22), (SEQS,), 1, ceiling + 1)
    ordering = jax.random.permutation(jax.random.fold_in(key, 23), SEQS)
    longest = jax.random.randint(jax.random.fold_in(key, 24), (), CTX - CTX_DEV // 2, top_len + 1)
    shortest = jax.random.randint(jax.random.fold_in(key, 25), (), 1, 2 * PROP + 1)
    lengths = lengths.at[ordering[0]].set(longest)
    lengths = lengths.at[ordering[1]].set(shortest)
    return lengths.astype(jnp.int32)


def draw_cache(key, part):
    sample = jnp.clip(jax.random.normal(jax.random.fold_in(key, 11), (SEQS, CTX, KV_RANK + ROPE), jnp.float32), -6.0, 6.0)
    lengths = shared_lengths(key)
    places = jnp.arange(CTX, dtype=jnp.int32)[None, :]
    recent = (places < lengths[:, None]) & (places >= lengths[:, None] - CTX_DEV // 4)
    boost = jnp.where(recent, 3.0, 1.0)[:, :, None]
    latent = sample[:, :, :KV_RANK] * boost
    sample = jnp.concatenate([latent, sample[:, :, KV_RANK:]], axis=-1)
    return sample.astype(jnp.bfloat16)


def draw_cached(key, part):
    return shared_lengths(key)


def draw_parents(key, part):
    limits = jnp.arange(1, PROP + 1, dtype=jnp.int32)
    picks = jax.random.randint(jax.random.fold_in(key, 31), (SEQS, PROP), 0, limits)
    parents = (picks - 1).astype(jnp.int32)
    deepest = jax.random.randint(jax.random.fold_in(key, 32), (), 0, SEQS)
    parents = parents.at[deepest, PROP - 1].set(PROP - 2)
    return parents.astype(jnp.int32)


def touch_ends(values, own_key, low, high):
    extent = values.shape
    place = [jax.random.randint(jax.random.fold_in(own_key, axis), (), 0, extent[axis]) for axis in range(len(extent))]
    values = values.at[tuple(place)].set(low)
    longest = extent.index(max(extent))
    place[longest] = (place[longest] + 1) % extent[longest]
    return values.at[tuple(place)].set(high)


def shard_levels(key, dims, split, least, high):
    level, own = 1.0, jax.random.fold_in(key, 6)
    for position, shards_of in split:
        heights = jnp.exp(jax.random.uniform(jax.random.fold_in(own, position), (shards_of,), jnp.float32, least / len(split), high / len(split)))
        level = level * jnp.repeat(heights, dims[position] // shards_of).reshape([-1 if axis == position else 1 for axis in range(len(dims))])
    return level


def centred(rng, shape, deviation, limit, split=(), kind=jnp.bfloat16):
    result = jax.random.normal(rng, shape, jnp.float32) * deviation
    if len(split) > 0:
        result = shard_levels(rng, shape, split, -0.22, 0.18) * result
    return jnp.clip(result, min=-limit, max=limit).astype(kind)


def setup_inputs(seed: int = 0) -> dict:
    keys = jax.random.split(jax.random.key(seed), 17)
    tokens = centred(keys[0], (SEQS, PROP, D), 1.0, 6.0)
    in_gain = jnp.clip(1.0 + 0.18 * jax.random.normal(keys[1], (D,), jnp.float32), 0.099609375, 1.8984375).astype(jnp.bfloat16)
    w_down_q = centred(keys[2], (D, Q_RANK), D ** -0.5, 0.125, ((0, 32),))
    w_down_kv = centred(keys[3], (D, KV_RANK), D ** -0.5, 0.125, ((0, 32),))
    w_rope_key = centred(keys[4], (D, ROPE), D ** -0.5, 0.125)
    q_gain = jnp.clip(1.0 + 0.18 * jax.random.normal(keys[5], (Q_RANK,), jnp.float32), 0.099609375, 1.8984375).astype(jnp.bfloat16)
    kv_gain = jnp.clip(1.0 + 0.18 * jax.random.normal(keys[6], (KV_RANK,), jnp.float32), 0.099609375, 1.8984375).astype(jnp.bfloat16)
    w_up_q = centred(keys[7], (Q_RANK, HEADS * (NOPE + ROPE)), Q_RANK ** -0.5, 0.25, ((1, 8),))
    w_absorb = centred(keys[8], (HEADS, NOPE, KV_RANK), NOPE ** -0.5, 0.75, ((0, 8),))
    w_value = centred(keys[9], (KV_RANK, HEADS * VDIM), KV_RANK ** -0.5, 0.375, ((1, 8),))
    w_out = centred(keys[10], (HEADS * VDIM, D), (HEADS * VDIM) ** -0.5, 0.1875, ((0, 8),))
    out_gain = jnp.clip(1.0 + 0.18 * jax.random.normal(keys[11], (D,), jnp.float32), 0.099609375, 1.8984375).astype(jnp.bfloat16)
    cache = draw_cache(jax.random.fold_in(keys[16], 71), 0)
    cached = draw_cached(jax.random.fold_in(keys[16], 71), 0)
    accepted = touch_ends(jax.random.randint(keys[14], (SEQS,), 0, PROP + 1), jax.random.fold_in(keys[14], 1), 0, PROP).astype(jnp.int32)
    parents = draw_parents(jax.random.fold_in(keys[16], 71), 0)
    return dict(tokens=tokens, in_gain=in_gain, w_down_q=w_down_q, w_down_kv=w_down_kv, w_rope_key=w_rope_key, q_gain=q_gain, kv_gain=kv_gain, w_up_q=w_up_q, w_absorb=w_absorb, w_value=w_value, w_out=w_out, out_gain=out_gain, cache=cache, cached=cached, accepted=accepted, parents=parents)


EPSILON = 1e-06
ROTARY_BASE = 10000.0
FLOOR_SCORE = -1e+30

def round_trip(values):
    return lax.optimization_barrier(values.astype(jnp.bfloat16)).astype(jnp.float32)

def rms_scale(values, gain_vec):
    floats = values.astype(jnp.float32)
    return floats * lax.rsqrt(lax.optimization_barrier(jnp.mean(floats * floats, axis=-1, keepdims=True)) + EPSILON) * gain_vec.astype(jnp.float32)

def rotate(values, positions):
    half_width = values.shape[-1] // 2
    frequency = ROTARY_BASE ** (-jnp.arange(half_width, dtype=jnp.float32) * 2.0 / values.shape[-1])
    angles = positions.astype(jnp.float32)[..., None] * frequency
    cosine = jnp.cos(angles)
    sine_part = jnp.sin(angles)
    lower_half = values[..., :half_width]
    upper_half = values[..., half_width:]
    return jnp.concatenate([lower_half * cosine - upper_half * sine_part, lower_half * sine_part + upper_half * cosine], axis=-1)

def ancestry(parents):
    num_prop = parents.shape[-1]
    slot_ids = jnp.arange(num_prop, dtype=jnp.int32)
    parent_hot = parents[:, :, None] == slot_ids[None, None, :]
    itself_mask = jnp.broadcast_to(slot_ids[:, None] == slot_ids[None, :], parent_hot.shape)
    reached = itself_mask
    for repeat in range(num_prop):
        reached = itself_mask | jnp.any(parent_hot[:, :, :, None] & reached[:, None, :, :], axis=2)
    return reached

def reference(tokens, in_gain, w_down_q, w_down_kv, w_rope_key, q_gain, kv_gain, w_up_q, w_absorb, w_value, w_out, out_gain, cache, cached, accepted, parents):
    f32 = jnp.float32
    bf16 = jnp.bfloat16
    normed = rms_scale(tokens, in_gain).astype(bf16).reshape(SEQS * PROP, D)
    query_in = rms_scale(jnp.dot(normed, w_down_q, preferred_element_type=f32), q_gain).astype(bf16)
    latent = rms_scale(jnp.dot(normed, w_down_kv, preferred_element_type=f32), kv_gain).astype(bf16)
    lengths = (cached + accepted).astype(jnp.int32)
    reached = ancestry(parents)
    depth_of = lax.optimization_barrier(jnp.sum(reached.astype(jnp.int32), axis=-1)) - 1
    positions = lengths[:, None] + depth_of
    rope_key = rotate(jnp.dot(normed, w_rope_key, preferred_element_type=f32).reshape(SEQS, PROP, ROPE), positions).astype(bf16)
    latent_rows = latent.reshape(SEQS, PROP, KV_RANK)
    new_rows = jnp.concatenate([latent_rows, rope_key], axis=-1)
    queries = jnp.dot(query_in, w_up_q, preferred_element_type=f32).reshape(SEQS, PROP, HEADS, NOPE + ROPE)
    query_nope = queries[..., :NOPE].astype(bf16)
    query_rope = rotate(queries[..., NOPE:], positions[:, :, None]).astype(bf16)
    query_lat = jnp.einsum('sphn,hnc->sphc', query_nope.astype(f32), w_absorb.astype(f32)).astype(bf16)
    score_scale = (NOPE + ROPE) ** (-0.5)
    key_pos = jnp.arange(CTX, dtype=jnp.int32)

    def one_sequence(seq_items):
        lat_q, rope_q, keys_all, length, reach_one, rows_one = seq_items
        keys_lat = keys_all[:, :KV_RANK].astype(f32)
        cache_scores = (jnp.einsum('phc,kc->phk', lat_q.astype(f32), keys_lat) + jnp.einsum('phr,kr->phk', rope_q.astype(f32), keys_all[:, KV_RANK:].astype(f32))) * score_scale
        visible = (key_pos < length).reshape(N_KV, CTX_DEV)
        blocked = cache_scores.reshape(PROP, HEADS, N_KV, CTX_DEV)
        masked = jnp.where(visible, blocked, FLOOR_SCORE)
        block_peak = lax.optimization_barrier(jnp.max(masked, axis=-1))
        weights = jnp.where(visible, jnp.exp(masked - block_peak[..., None]), 0.0)
        block_den = lax.optimization_barrier(jnp.sum(weights, axis=-1))
        block_num = jnp.einsum('phbk,bkc->phbc', round_trip(weights), keys_lat.reshape(N_KV, CTX_DEV, KV_RANK))
        rows_lat = rows_one[:, :KV_RANK].astype(f32)
        prop_scores = (jnp.einsum('phc,kc->phk', lat_q.astype(f32), rows_lat) + jnp.einsum('phr,kr->phk', rope_q.astype(f32), rows_one[:, KV_RANK:].astype(f32))) * score_scale
        allowed = reach_one[:, None, :]
        prop_masked = jnp.where(allowed, prop_scores, FLOOR_SCORE)
        prop_peak = lax.optimization_barrier(jnp.max(prop_masked, axis=-1))
        prop_weights = jnp.where(allowed, jnp.exp(prop_masked - prop_peak[..., None]), 0.0)
        prop_den = lax.optimization_barrier(jnp.sum(prop_weights, axis=-1))
        prop_num = jnp.einsum('phk,kc->phc', round_trip(prop_weights), rows_lat)
        highest = jnp.maximum(lax.optimization_barrier(jnp.max(block_peak, axis=-1)), prop_peak)
        block_factor = jnp.exp(block_peak - highest[..., None])
        prop_factor = jnp.exp(prop_peak - highest)
        numerator = lax.optimization_barrier(jnp.sum(block_num * block_factor[..., None], axis=2)) + prop_num * prop_factor[..., None]
        denominator = lax.optimization_barrier(jnp.sum(block_den * block_factor, axis=-1)) + prop_den * prop_factor
        return (numerator / denominator[..., None]).astype(bf16)
    lat_out = lax.map(one_sequence, (query_lat, query_rope, cache, lengths, reached, new_rows))
    head_out = jnp.einsum('sphc,chv->sphv', lat_out.astype(f32), w_value.reshape(KV_RANK, HEADS, VDIM).astype(f32)).astype(bf16)
    per_group = HEADS // N_TP
    grouped = head_out.reshape(SEQS * PROP, N_TP, per_group * VDIM)
    out_rows = w_out.reshape(N_TP, per_group * VDIM, D)
    partials = jnp.einsum('tgc,gcd->gtd', grouped.astype(f32), out_rows.astype(f32))
    summed = lax.optimization_barrier(jnp.sum(round_trip(partials), axis=0))
    attended = rms_scale(summed, out_gain).astype(bf16).reshape(SEQS, PROP, D)
    slot_ids = key_pos[None, :] - lengths[:, None]
    onehot = (slot_ids[:, :, None] == jnp.arange(PROP, dtype=jnp.int32)[None, None, :]).astype(f32)
    placed = jnp.einsum('skp,spc->skc', onehot, new_rows.astype(f32)).astype(bf16)
    inside = (slot_ids >= 0) & (slot_ids < PROP)
    new_cache = jnp.where(inside[:, :, None], placed, cache)
    return (attended, new_cache)
```

```python
import functools

import jax
import jax.numpy as jnp
from jax import lax
from jax.experimental import pallas as pl
from jax.experimental.pallas import tpu as pltpu
from jax.sharding import Mesh
from jax.sharding import PartitionSpec as P

KV = ("kv_0", "kv_1")
MESH = pl.DeviceIdType.MESH

EPSILON = 1e-06
ROTARY_BASE = 10000.0
FLOOR_SCORE = -1e30
NZ, NY, NT = 8, 4, 8
LANES = 128
KEPT = 16 * 1024 * 1024
F32 = jnp.float32
BF16 = jnp.bfloat16
NT_DIMS = (((1,), (1,)), ((), ()))


def ancestry(parents):
    num_prop = parents.shape[-1]
    slot_ids = jnp.arange(num_prop, dtype=jnp.int32)
    parent_hot = parents[:, :, None] == slot_ids[None, None, :]
    itself_mask = jnp.broadcast_to(slot_ids[:, None] == slot_ids[None, :], parent_hot.shape)
    reached = itself_mask
    for repeat in range(num_prop):
        reached = itself_mask | jnp.any(parent_hot[:, :, :, None] & reached[:, None, :, :], axis=2)
    return reached


def wait_for(ref, sem):
    pltpu.make_async_copy(ref, ref, sem).wait()


def down_kernel(
    tokens_ref, gain_ref, wq_ref, wkv_ref, wrope_ref, qgain_ref, kvgain_ref, cos_ref, sin_ref,
    out_ref,
    normed, parts, from_z, y_sum, from_y, cols, own, gathered,
    z_send, z_recv, y_send, y_recv, c_send, c_recv, t_send, t_recv,
):
    z, y, t = lax.axis_index("kv_0"), lax.axis_index("kv_1"), lax.axis_index("tp")
    blocks = cols.shape[0]
    q_blocks = wq_ref.shape[1] // LANES
    q_width, kv_width = wq_ref.shape[1], wkv_ref.shape[1]
    barrier = pltpu.get_barrier_semaphore()
    for d in range(1, NZ):
        pl.semaphore_signal(barrier, inc=1, device_id={"kv_0": lax.rem(z + d, NZ)}, device_id_type=MESH)
    for d in range(1, NY):
        pl.semaphore_signal(barrier, inc=1, device_id={"kv_1": lax.rem(y + d, NY)}, device_id_type=MESH)
    for d in range(1, NT):
        pl.semaphore_signal(barrier, inc=1, device_id={"tp": lax.rem(t + d, NT)}, device_id_type=MESH)

    x = tokens_ref[t].astype(F32)
    x = x * lax.rsqrt(jnp.mean(x * x, axis=-1, keepdims=True) + EPSILON) * gain_ref[...].astype(F32)[None, :]
    normed[...] = x.astype(BF16)
    rows = wq_ref.shape[0]
    kv = z * NY + y
    window = normed[:, pl.ds(pl.multiple_of(kv // 2 * LANES, LANES), LANES)]
    lane = lax.broadcasted_iota(jnp.int32, window.shape, 1)
    window = jnp.where(lane // rows == lax.rem(kv, 2), window.astype(F32), 0.0).astype(BF16)
    part_q = jnp.dot(window, jnp.concatenate([wq_ref[...]] * 2, axis=0), preferred_element_type=F32)
    part_kv = jnp.dot(window, jnp.concatenate([wkv_ref[...]] * 2, axis=0), preferred_element_type=F32)
    for c in range(q_blocks):
        parts[c] = part_q[:, c * LANES : (c + 1) * LANES]
    for c in range(blocks - q_blocks):
        parts[q_blocks + c] = part_kv[:, c * LANES : (c + 1) * LANES]
    pl.semaphore_wait(barrier, NZ + NY + NT - 3)

    def z_copy(d):
        to = lax.rem(z + d, NZ)
        return to, pltpu.make_async_remote_copy(
            src_ref=parts.at[lax.rem(to, blocks)], dst_ref=from_z.at[d - 1],
            send_sem=z_send.at[d - 1], recv_sem=z_recv.at[d - 1],
            device_id={"kv_0": to}, device_id_type=MESH)

    for d in range(1, NZ):
        to, copy = z_copy(d)
        pl.when(to < blocks)(copy.start)

    half = wrope_ref.shape[0] // 2
    low = lax.dot_general(normed[...], wrope_ref[0:half, :], NT_DIMS, preferred_element_type=F32)
    high = lax.dot_general(normed[...], wrope_ref[half:, :], NT_DIMS, preferred_element_type=F32)
    cosine, sine = cos_ref[t], sin_ref[t]
    rope = jnp.concatenate(
        [low * cosine - high * sine, low * sine + high * cosine,
         jnp.zeros((low.shape[0], LANES - 2 * half), F32)], axis=-1).astype(BF16)

    @pl.when(z < blocks)
    def _():
        total = parts[lax.rem(z, blocks)]
        for d in range(1, NZ):
            wait_for(from_z.at[d - 1], z_recv.at[d - 1])
        for d in range(1, NZ):
            total = total + from_z[d - 1]
        y_sum[...] = total
        for d in range(1, NY):
            pltpu.make_async_remote_copy(
                src_ref=y_sum, dst_ref=from_y.at[d - 1], send_sem=y_send.at[d - 1], recv_sem=y_recv.at[d - 1],
                device_id={"kv_1": lax.rem(y + d, NY)}, device_id_type=MESH).start()
        for d in range(1, NY):
            wait_for(from_y.at[d - 1], y_recv.at[d - 1])
        terms = [y_sum[...]] + [from_y[d - 1] for d in range(1, NY)]
        whole = jnp.zeros_like(total)
        for owner in range(NY):
            back = lax.rem(y - owner + NY, NY)
            pick = terms[0]
            for d in range(1, NY):
                pick = jnp.where(back == d, terms[d], pick)
            whole = whole + pick
        cols[lax.rem(z, blocks)] = whole
        for d in range(1, NZ):
            pltpu.make_async_remote_copy(
                src_ref=cols.at[lax.rem(z, blocks)], dst_ref=cols.at[lax.rem(z, blocks)],
                send_sem=c_send.at[d - 1], recv_sem=c_recv.at[lax.rem(z, blocks)],
                device_id={"kv_0": lax.rem(z + d, NZ)}, device_id_type=MESH).start()

    for c in range(blocks):
        @pl.when(z != c)
        def _():
            wait_for(cols.at[c], c_recv.at[c])

    def scaled(first, count, width, gain):
        values = [cols[first + c] for c in range(count)]
        squares = values[0] * values[0]
        for v in values[1:]:
            squares = squares + v * v
        factor = lax.rsqrt(jnp.sum(squares, axis=-1, keepdims=True) / width + EPSILON)
        return jnp.concatenate(
            [v * factor * gain[:, c * LANES : (c + 1) * LANES] for c, v in enumerate(values)],
            axis=-1).astype(BF16)

    ready = jnp.concatenate(
        [scaled(0, q_blocks, q_width, qgain_ref[...].astype(F32)[None, :]),
         scaled(q_blocks, blocks - q_blocks, kv_width, kvgain_ref[...].astype(F32)[None, :]), rope], axis=-1)
    for i in range(own.shape[0]):
        own[i] = ready[8 * i : 8 * i + 8]
    for d in range(1, NT):
        pltpu.make_async_remote_copy(
            src_ref=own, dst_ref=gathered.at[t], send_sem=t_send.at[d - 1], recv_sem=t_recv.at[t],
            device_id={"tp": lax.rem(t + d, NT)}, device_id_type=MESH).start()
    out_ref[t] = own[...]
    for d in range(1, NT):
        src = lax.rem(t + d, NT)
        wait_for(gathered.at[src], t_recv.at[src])
        out_ref[src] = gathered[src]

    for d in range(1, NZ):
        to, copy = z_copy(d)
        pl.when(to < blocks)(copy.wait_send)
    @pl.when(z < blocks)
    def _():
        for d in range(1, NY):
            wait_for(y_sum, y_send.at[d - 1])
        for d in range(1, NZ):
            wait_for(cols.at[0], c_send.at[d - 1])
    for d in range(1, NT):
        wait_for(own, t_send.at[d - 1])


def down(tokens, in_gain, w_q, w_kv, w_rope_t, q_gain, kv_gain, cosine, sine):
    per, width = tokens.shape[1], tokens.shape[2]
    blocks = (w_q.shape[1] + w_kv.shape[1]) // LANES
    total = (blocks + 1) * LANES
    vmem = pl.BlockSpec(memory_space=pltpu.VMEM)
    dma = pltpu.SemaphoreType.DMA
    return pl.pallas_call(
        down_kernel,
        out_shape=jax.ShapeDtypeStruct((NT, per // 8, 8, total), BF16),
        in_specs=[vmem] * 9,
        out_specs=vmem,
        scratch_shapes=[
            pltpu.VMEM((per, width), BF16),
            pltpu.VMEM((blocks, per, LANES), F32),
            pltpu.VMEM((NZ - 1, per, LANES), F32),
            pltpu.VMEM((per, LANES), F32),
            pltpu.VMEM((NY - 1, per, LANES), F32),
            pltpu.VMEM((blocks, per, LANES), F32),
            pltpu.VMEM((per // 8, 8, total), BF16),
            pltpu.VMEM((NT, per // 8, 8, total), BF16),
            dma((NZ - 1,)), dma((NZ - 1,)), dma((NY - 1,)), dma((NY - 1,)),
            dma((NZ - 1,)), dma((blocks,)), dma((NT - 1,)), dma((NT,)),
        ],
        compiler_params=pltpu.CompilerParams(collective_id=0, has_side_effects=True),
        name="down",
    )(tokens, in_gain, w_q, w_kv, w_rope_t, q_gain, kv_gain, cosine, sine)


def as_row(column):
    rows = lax.broadcasted_iota(jnp.int32, (16, LANES), 0)
    lanes = lax.broadcasted_iota(jnp.int32, (16, LANES), 1)
    return jnp.sum(jnp.where(rows == lanes, jnp.broadcast_to(column, (16, LANES)), 0.0), axis=0, keepdims=True)


def split3(x):
    high = x.astype(BF16).astype(F32)
    rest = x - high
    middle = rest.astype(BF16).astype(F32)
    return high, middle, rest - middle


def with_stats(num, top, den):
    top, den = split3(top), split3(den)
    row = lax.broadcasted_iota(jnp.int32, num.shape, 0)
    pair = [jnp.concatenate(p, axis=-1) for p in ((top[0], top[1]), (top[2], den[0]), (den[1], den[2]))]
    return jnp.where(row == 6, pair[0], jnp.where(row == 7, pair[1], jnp.where(row == 14, pair[2], num))).astype(BF16)


def stats_of(block):
    return (
        block[6:7, :LANES] + block[6:7, LANES:] + block[7:8, :LANES],
        block[7:8, LANES:] + block[14:15, :LANES] + block[14:15, LANES:],
    )


AHEAD = 8


def cache_kernel(scale, start_ref, q_ref, rows_ref, cache_ref, new_ref, block_ref, slots, r_sem, w_sem):
    seqs, _, span = slots.shape
    latent = block_ref.shape[2]
    num_prop = 6

    def read(s):
        return pltpu.make_async_copy(cache_ref.at[s], slots.at[s], r_sem.at[s])

    def write(s):
        return pltpu.make_async_copy(slots.at[s], new_ref.at[s], w_sem.at[s])

    def attend(s, start, n):
        scores = jnp.dot(q_ref[s], slots[s, :, 0:n], preferred_element_type=F32) * scale
        seen = lax.broadcasted_iota(jnp.int32, scores.shape, 1) < start
        masked = jnp.where(seen, scores, FLOOR_SCORE)
        top = jnp.max(masked, axis=-1, keepdims=True)
        weights = jnp.where(seen, jnp.exp(masked - top), 0.0)
        den = jnp.sum(weights, axis=-1, keepdims=True)
        num = lax.dot_general(
            weights.astype(BF16), slots[s, 0:latent, 0:n], NT_DIMS, preferred_element_type=F32)
        block_ref[s] = with_stats(num, as_row(top), as_row(den))

    def step(s, carry):
        @pl.when(s + AHEAD < seqs)
        def _():
            read(s + AHEAD).start()

        read(s).wait()
        start = start_ref[s]

        @pl.when(start <= 0)
        def _():
            block_ref[s] = with_stats(
                jnp.zeros((16, latent), F32), jnp.full((1, LANES), FLOOR_SCORE, F32), jnp.zeros((1, LANES), F32))

        least = 0
        for n in (span // 8, span // 2, span):
            @pl.when((start > least) & ((start <= n) | (n == span)))
            def _():
                attend(s, start, n)
            least = n

        @pl.when((start > -num_prop) & (start < span))
        def _():
            wide = 2 * LANES
            base = jnp.minimum(jnp.maximum(start, 0) // LANES * LANES, span - wide)
            base = pl.multiple_of(base, LANES)
            old = slots[s, :, pl.ds(base, wide)]
            which = lax.broadcasted_iota(jnp.int32, (16, wide), 1) + base - start
            slot = lax.broadcasted_iota(jnp.int32, (16, wide), 0)
            hot = jnp.where((which == slot) & (slot < num_prop), 1.0, 0.0).astype(BF16)
            placed = lax.dot_general(rows_ref[s], hot, (((0,), (0,)), ((), ())), preferred_element_type=F32)
            at = lax.broadcasted_iota(jnp.int32, placed.shape, 1) + base - start
            fresh = jnp.where((at >= 0) & (at < num_prop), placed, old.astype(F32))
            slots[s, :, pl.ds(base, wide)] = fresh.astype(BF16)

        write(s).start()
        return carry

    def written(s, carry):
        write(s).wait()
        return carry

    for s in range(AHEAD):
        read(s).start()
    lax.fori_loop(0, seqs, step, 0)
    lax.fori_loop(0, seqs, written, 0)


def cache_step(start, queries, rows, cache_t, latent, scale):
    seqs = cache_t.shape[0]
    vmem, anywhere = pl.BlockSpec(memory_space=pltpu.VMEM), pl.BlockSpec(memory_space=pl.ANY)
    return pl.pallas_call(
        functools.partial(cache_kernel, scale),
        out_shape=(
            jax.ShapeDtypeStruct(cache_t.shape, BF16),
            jax.ShapeDtypeStruct((seqs, 16, latent), BF16),
        ),
        in_specs=[pl.BlockSpec(memory_space=pltpu.SMEM), vmem, vmem, anywhere],
        out_specs=(anywhere, vmem),
        scratch_shapes=[
            pltpu.VMEM(cache_t.shape, BF16),
            pltpu.SemaphoreType.DMA((seqs,)),
            pltpu.SemaphoreType.DMA((seqs,)),
        ],
        compiler_params=pltpu.CompilerParams(vmem_limit_bytes=3 * KEPT),
        name="cache_step",
    )(start, queries, rows, cache_t)


def combine_kernel(
    scale,
    block_ref, q_ref, rows_ref, allowed_ref, wv_ref, wo_ref, gain_ref,
    out_ref,
    arrived, tops, dens, partial, parts, done, final,
    a_send, a_recv, p_send, p_recv, f_send, f_recv,
):
    z, y, t = lax.axis_index("kv_0"), lax.axis_index("kv_1"), lax.axis_index("tp")
    kv = z * NY + y
    n_kv = NZ * NY
    latent = block_ref.shape[2]
    barrier = pltpu.get_barrier_semaphore()

    def peer(d):
        other = lax.rem(kv + d, n_kv)
        return other, {"kv_0": other // NY, "kv_1": lax.rem(other, NY)}

    def greet(d, carry):
        _, where_to = peer(d)
        pl.semaphore_signal(barrier, inc=1, device_id=where_to, device_id_type=MESH)
        return carry

    lax.fori_loop(1, n_kv, greet, 0)
    for d in range(1, NT):
        pl.semaphore_signal(barrier, inc=1, device_id={"tp": lax.rem(t + d, NT)}, device_id_type=MESH)
    pl.semaphore_wait(barrier, n_kv - 1 + NT - 1)

    def send(d, carry):
        other, where_to = peer(d)
        pltpu.make_async_remote_copy(
            src_ref=block_ref.at[other], dst_ref=arrived.at[d - 1], send_sem=a_send.at[d - 1],
            recv_sem=a_recv.at[d - 1], device_id=where_to, device_id_type=MESH).start()
        return carry

    lax.fori_loop(1, n_kv, send, 0)

    rows = rows_ref[kv]
    prop_scores = lax.dot_general(q_ref[kv], rows, NT_DIMS, preferred_element_type=F32) * scale
    allowed = allowed_ref[...] > 0.5
    prop_masked = jnp.where(allowed, prop_scores, FLOOR_SCORE)
    prop_top = jnp.max(prop_masked, axis=-1, keepdims=True)
    prop_weights = jnp.where(allowed, jnp.exp(prop_masked - prop_top), 0.0)
    prop_den = jnp.sum(prop_weights, axis=-1, keepdims=True)
    prop_num = jnp.dot(prop_weights.astype(BF16), rows[:, 0:latent], preferred_element_type=F32)
    own = block_ref[kv].astype(F32)
    own_top, own_den = stats_of(own)
    prop_top_row, prop_den_row = as_row(prop_top), as_row(prop_den)
    eye = lax.broadcasted_iota(jnp.int32, (16, LANES), 0) == lax.broadcasted_iota(jnp.int32, (16, LANES), 1)

    def as_column(row):
        return jnp.sum(jnp.where(eye, jnp.broadcast_to(row, (16, LANES)), 0.0), axis=-1, keepdims=True)

    def arrive(d, carry):
        wait_for(arrived.at[d - 1], a_recv.at[d - 1])
        return carry

    lax.fori_loop(1, n_kv, arrive, 0)

    for d in range(n_kv - 1):
        top, den = stats_of(arrived[d].astype(F32))
        tops[d : d + 1], dens[d : d + 1] = top, den
    tops[n_kv - 1 : n_kv], dens[n_kv - 1 : n_kv] = own_top, own_den
    highest = jnp.maximum(prop_top_row, jnp.max(tops[...], axis=0, keepdims=True))
    factors = jnp.exp(tops[...] - highest)
    prop_factor = jnp.exp(prop_top_row - highest)
    den_row = jnp.sum(dens[...] * factors, axis=0, keepdims=True) + prop_den_row * prop_factor
    num = own * as_column(factors[n_kv - 1 : n_kv]) + prop_num * as_column(prop_factor)
    for d in range(n_kv - 1):
        num = num + arrived[d].astype(F32) * as_column(factors[d : d + 1])
    den = as_column(den_row)
    real = lax.rem(lax.broadcasted_iota(jnp.int32, num.shape, 0), 8) < 6
    lat_out = jnp.where(real, num / den, 0.0).astype(BF16)
    by_head = jnp.dot(lat_out, wv_ref[...], preferred_element_type=F32)
    lane = lax.broadcasted_iota(jnp.int32, (8, by_head.shape[1]), 1)
    head_out = jnp.where(lane < by_head.shape[1] // 2, by_head[0:8], by_head[8:16]).astype(BF16)
    partial[...] = jnp.dot(head_out, wo_ref[...], preferred_element_type=F32).astype(BF16)

    def p_copy():
        return pltpu.make_async_remote_copy(
            src_ref=partial, dst_ref=parts.at[t], send_sem=p_send, recv_sem=p_recv.at[t],
            device_id={"tp": z}, device_id_type=MESH)

    @pl.when(t != z)
    def _():
        p_copy().start()

    def f_copy(d):
        _, where_to = peer(d)
        return pltpu.make_async_remote_copy(
            src_ref=done, dst_ref=final.at[y], send_sem=f_send.at[d - 1], recv_sem=f_recv.at[y],
            device_id=where_to, device_id_type=MESH)

    @pl.when(t == z)
    def _():
        for g in range(NT):
            @pl.when(t != g)
            def _():
                wait_for(parts.at[g], p_recv.at[g])
        parts[t] = partial[...]
        summed = parts[0].astype(F32)
        for g in range(1, NT):
            summed = summed + parts[g].astype(F32)
        normed = summed * lax.rsqrt(jnp.mean(summed * summed, axis=-1, keepdims=True) + EPSILON)
        done[...] = (normed * gain_ref[...].astype(F32)[None, :]).astype(BF16)

        def spread(d, carry):
            f_copy(d).start()
            return carry

        lax.fori_loop(1, n_kv, spread, 0)
        final[y] = done[...]

    for i in range(NY):
        @pl.when((t != z) | (y != i))
        def _():
            wait_for(final.at[i], f_recv.at[i])
    out_ref[...] = final[...]

    def sent(d, carry):
        wait_for(block_ref.at[0], a_send.at[d - 1])
        return carry

    lax.fori_loop(1, n_kv, sent, 0)

    @pl.when(t != z)
    def _():
        p_copy().wait_send()

    @pl.when(t == z)
    def _():
        def spread_sent(d, carry):
            f_copy(d).wait_send()
            return carry

        lax.fori_loop(1, n_kv, spread_sent, 0)


def combine(blocks, queries, rows, allowed, w_value, w_out, out_gain, scale):
    n_kv = NZ * NY
    latent, width = blocks.shape[2], w_out.shape[1]
    vmem = pl.BlockSpec(memory_space=pltpu.VMEM)
    dma = pltpu.SemaphoreType.DMA
    return pl.pallas_call(
        functools.partial(combine_kernel, scale),
        out_shape=jax.ShapeDtypeStruct((NY, 8, width), BF16),
        in_specs=[vmem] * 7,
        out_specs=vmem,
        scratch_shapes=[
            pltpu.VMEM((n_kv - 1, 16, latent), BF16),
            pltpu.VMEM((n_kv, LANES), F32),
            pltpu.VMEM((n_kv, LANES), F32),
            pltpu.VMEM((8, width), BF16),
            pltpu.VMEM((NT, 8, width), BF16),
            pltpu.VMEM((8, width), BF16),
            pltpu.VMEM((NY, 8, width), BF16),
            dma((n_kv - 1,)), dma((n_kv - 1,)), dma, dma((NT,)), dma((n_kv - 1,)), dma((NY,)),
        ],
        compiler_params=pltpu.CompilerParams(collective_id=1, has_side_effects=True, vmem_limit_bytes=KEPT),
        name="combine",
    )(blocks, queries, rows, allowed, w_value, w_out, out_gain)


def local(
    tokens, in_gain, w_down_q, w_down_kv, w_rope_key, q_gain, kv_gain, w_up_q, w_absorb, w_value, w_out,
    out_gain, cache, cached, accepted, parents,
):
    num_seqs, num_prop, model_width = tokens.shape
    num_rows = num_seqs * num_prop
    q_rank, latent_width = w_down_q.shape[1], w_down_kv.shape[1]
    rope_width = w_rope_key.shape[1]
    local_heads, nope_width = w_absorb.shape[0], w_absorb.shape[1]
    local_span = cache.shape[1]
    half = rope_width // 2
    scale = (nope_width + rope_width) ** (-0.5)
    kv = lax.axis_index(KV)

    lengths = cached + accepted
    reached = ancestry(parents)
    positions = lengths[:, None] + jnp.sum(reached.astype(jnp.int32), axis=-1) - 1
    frequency = ROTARY_BASE ** (-jnp.arange(half, dtype=F32) * 2.0 / rope_width)
    angles = positions.T.astype(F32)[..., None] * frequency
    cosine = jnp.cos(angles).reshape(num_rows, half)
    sine = jnp.sin(angles).reshape(num_rows, half)

    flat_tokens = jnp.swapaxes(tokens, 0, 1).reshape(NT, num_rows // NT, model_width)
    shared = down(
        flat_tokens, in_gain, w_down_q, w_down_kv, w_rope_key.T, q_gain, kv_gain,
        cosine.reshape(NT, num_rows // NT, half), sine.reshape(NT, num_rows // NT, half),
    ).reshape(num_rows, -1)
    query_in = shared[:, :q_rank]
    new_rows = shared[:, q_rank : q_rank + latent_width + rope_width]

    queries = jnp.dot(query_in, w_up_q, preferred_element_type=F32)
    by_head = []
    for h in range(local_heads):
        own = queries[:, h * (nope_width + rope_width) : (h + 1) * (nope_width + rope_width)]
        nope = own[:, :nope_width].astype(BF16)
        low, high = own[:, nope_width : nope_width + half], own[:, nope_width + half :]
        lat = jnp.dot(nope, w_absorb[h], preferred_element_type=F32).astype(BF16)
        full = jnp.concatenate(
            [lat, (low * cosine - high * sine).astype(BF16), (low * sine + high * cosine).astype(BF16)], axis=-1)
        by_head.append(jnp.pad(full.reshape(num_prop, num_seqs, -1), ((0, 8 - num_prop), (0, 0), (0, 0))))
    full_query = jnp.swapaxes(jnp.concatenate(by_head, axis=0), 0, 1)
    rows = jnp.pad(new_rows.reshape(num_prop, num_seqs, -1), ((0, 16 - num_prop), (0, 0), (0, 0)))
    rows = jnp.swapaxes(rows, 0, 1)

    start = lengths - kv * local_span
    new_cache, blocks = cache_step(
        start, full_query, rows, jnp.swapaxes(cache, 1, 2), latent_width, scale)

    mine = lax.dynamic_index_in_dim(reached, kv, 0, keepdims=False).astype(F32)
    mine = jnp.pad(mine, ((0, 8 - num_prop), (0, 16 - num_prop)))
    allowed = jnp.concatenate([mine] * local_heads, axis=0)
    attended = combine(blocks, full_query, rows, allowed, w_value, w_out, out_gain, scale)
    return attended[:, :num_prop], jnp.swapaxes(new_cache, 1, 2)


def solution(mesh):
    torus = Mesh(mesh.devices.reshape(NZ, NY, NT), ("kv_0", "kv_1", "tp"))
    in_specs = (
        P(), P(), P(KV, None), P(KV, None), P(), P(), P(), P(None, "tp"), P("tp", None, None), P(None, "tp"),
        P("tp", None), P(), P(None, KV, None), P(), P(), P(),
    )
    out_specs = (P("tp", None, None), P(None, KV, None))
    return jax.shard_map(local, mesh=torus, in_specs=in_specs, out_specs=out_specs, check_vma=False)
```
